512 devices in a mesh: ep: 32 (over z, core), tp: 16 (over y, x).
Axes of the slice: x: 4, y: 4, z: 16, core: 2. Of those that a mesh axis runs over, the one named last changes fastest.
Arguments:
- q_latent: bfloat16 [16384, 512], P('ep'), may hold values from -6 to 6
- kv_latent: bfloat16 [16384, 256], P('ep'), may hold values from -6 to 6
- rope_key: bfloat16 [16384, 32], P('ep'), may hold values from -400 to 400
- q_gain: bfloat16 [512], replicated, may hold values from 0.099609375 to 1.8984375
- kv_gain: bfloat16 [256], replicated, may hold values from 0.099609375 to 1.8984375
- w_q_nope: bfloat16 [512, 1024], P(None, 'tp'), may hold values from -0.25 to 0.25
- w_q_rope: bfloat16 [512, 512], P(None, 'tp'), may hold values from -0.25 to 0.25
- w_k_nope: bfloat16 [256, 1024], P(None, 'tp'), may hold values from -0.375 to 0.375
- w_value: bfloat16 [256, 1024], P(None, 'tp'), may hold values from -0.375 to 0.375
- w_out: bfloat16 [1024, 2048], P('tp'), may hold values from -5.375 to 5.375
- tokens_b: bfloat16 [4096, 2048], P('ep'), may hold values from -6 to 6
- norm_gain_b: bfloat16 [2048], replicated, may hold values from 0.099609375 to 1.8984375
- routes: int32 [4096, 2], P('ep'), may hold values from 0 to 31, all different within a row; in each aligned block of 128 rows (0 to 127, 128 to 255, ...) at most 12 rows name the same one
- route_logits: float32 [4096, 2], P('ep'), may hold values from -6 to 6
- w_gate: bfloat16 [32, 2048, 4096], P('ep', None, 'tp'), may hold values from -0.125 to 0.125
- w_up: bfloat16 [32, 2048, 4096], P('ep', None, 'tp'), may hold values from -0.125 to 0.125
- w_down: bfloat16 [32, 4096, 2048], P('ep', 'tp'), may hold values from -0.125 to 0.125
Outputs:
- mixer_out: bfloat16 [16384, 2048], P(('ep', 'tp'))
- expert_mix: bfloat16 [4096, 2048], P('ep', 'tp')
The draws below stay inside these ranges and needn't reach their ends.
Inputs may be any that keep to these rules, and one draw needn't show every extreme that they name: `routes`: each row names two different experts. In each aligned block of 128 rows (the rows of one index of ep) no expert is named by more than 12 rows, and in every draw some expert is named by exactly 12 rows of some block.
All inputs are finite; a program needn't handle non-finite values.
Results may differ from the reference program's by a relative error of at most 0.022.
The reference program's roundings to bfloat16 on the way count: a program that leaves them out, or rounds other values in their place, can miss the bound.
Values may be sent and summed in bfloat16 or wider, within the bound.
No kernel may reach another device: no remote copies, remote signals or barrier semaphores. Data moves between devices by JAX's collectives and lax.ppermute only.
A program may use at most 128 MiB of HBM per device.

```python
import math
import jax
import jax.numpy as jnp
import numpy as np
from jax import lax

D = 2048
HEADS = 16
NOPE = 64
ROPE = 32
VDIM = 64
QLAT = 512
KVLAT = 256
FFE = 4096
R_B = 128
TOK_A = 16384
TOK_B = 4096
EXPERTS = 32
CAP = 12
N_EP = 32
N_TP = 16


def draw_rope_key(key, part):
    base = jax.random.normal(jax.random.fold_in(key, 11), (TOK_A, ROPE), jnp.float32)
    return jnp.clip(base, -400.0, 400.0).astype(jnp.bfloat16)


def with_spikes(drawn, stream_key, source, target, blocks, factor):
    owner, partner = [(jnp.arange(drawn.shape[axis_at]) // (drawn.shape[axis_at] // blocks)).reshape([-1 if axis == axis_at else 1 for axis in range(drawn.ndim)]) for axis_at in (source, target)]
    chosen = jax.random.permutation(stream_key, blocks)[partner]
    strong = (owner == chosen) | (owner == (partner + blocks // 2) % blocks)
    return jnp.where(strong, factor * drawn, drawn)


def level_of(own_key, extent, cuts, low, top_value):
    level = 1.0
    for axis_at, blocks in cuts:
        steps = jax.random.uniform(jax.random.fold_in(jax.random.fold_in(own_key, 6), axis_at), (blocks,), jnp.float32, low / len(cuts), top_value / len(cuts))
        level = level * jnp.repeat(jnp.exp(steps), extent[axis_at] // blocks).reshape((-1,) + (1,) * (len(extent) - 1 - axis_at))
    return level


def assign_block(stream_key, own, number, rows, number_of, top, most, slope):
    ranking = jax.random.permutation(stream_key, number_of)
    crowded, usual = load_shares(number_of, rows * top, most, slope, True), load_shares(number_of, rows * top, most, slope, False)
    places = jnp.arange(number_of)

    def named(sizes, turn):
        used = int((sizes > 0).sum())
        fixed = max(1, used // 4)
        passed = fixed + (places - fixed + turn * (used - fixed)) % max(1, number_of - fixed)
        return jnp.zeros((number_of,), jnp.int32).at[ranking[jnp.where(places < fixed, places, passed)]].set(jnp.asarray(sizes, jnp.int32))

    sizes = jnp.where(number % 4 == 0, named(crowded, number // 4), named(usual, number - number // 4 - 1))
    mixed = jax.random.permutation(jax.random.fold_in(own, 3), number_of)
    donor, sink = mixed[0:number_of // 2 * 2:2], mixed[1:number_of // 2 * 2:2]
    margin = jnp.minimum(sizes[donor] - 1, most - sizes[sink]) // 2
    margin = jnp.where((donor == ranking[0]) | (sink == ranking[0]) | (sizes[sink] == 0), 0, jnp.maximum(margin, 0))
    passed = jax.random.randint(jax.random.fold_in(own, 4), (number_of // 2,), 0, 1 << 20) % (margin + 1)
    sizes = sizes.at[donor].add(-passed).at[sink].add(passed)
    items = jnp.searchsorted(jnp.cumsum(sizes), jnp.arange(rows * top), side="right").astype(jnp.int32)
    grid = items.reshape(top, rows).T
    grid = grid[jax.random.permutation(jax.random.fold_in(own, 1), rows)]
    turn = jax.random.randint(jax.random.fold_in(own, 2), (rows, 1), 0, top)
    return jnp.take_along_axis(grid, (jnp.arange(top)[None, :] + turn) % top, axis=1)


def load_shares(count, total, reach, skew, full):
    loads = [(1 << 20) // math.isqrt(grade ** skew) + 1 for grade in range(1, count + 1)]
    largest = reach if full else min(reach, max(-(-total // count), total * loads[0] // sum(loads)))
    least = 1 if total - largest >= count - 1 else 0
    given, rest = [largest] + [least] * (count - 1), total - largest - least * (count - 1)
    while rest > 0:
        candidates = [i for i in range(1, count) if given[i] < largest] or [i for i in range(1, count) if given[i] < reach]
        pool, remaining = sum([loads[i] for i in candidates]), rest
        for i in candidates:
            more = min(reach - given[i], max(1, remaining * loads[i] // pool), rest)
            given[i] = given[i] + more
            rest = rest - more
    return np.array(given)


def centred(key, shape, scale, most, cuts=(), kind=jnp.bfloat16):
    entries = jax.random.normal(key, shape, jnp.float32) * scale
    if len(cuts) > 0:
        entries = level_of(key, shape, cuts, -0.22, 0.18) * entries
    return jnp.clip(entries, min=-most, max=most).astype(kind)


def noise_with(key, extent, width, bound, pieces, heavy, kind=jnp.bfloat16):
    drawn = width * jax.random.normal(key, extent, jnp.float32)
    if pieces:
        drawn = drawn * level_of(key, extent, pieces, -0.22, 0.18)
    return jnp.clip(with_spikes(drawn, jax.random.fold_in(key, 3), *heavy), -bound, bound).astype(kind)


def setup_inputs(seed: int = 0) -> dict:
    keys = jax.random.split(jax.random.key(seed), 18)
    q_latent = centred(keys[0], (TOK_A, QLAT), 1.0, 6.0, ((0, 32),))
    kv_latent = centred(keys[1], (TOK_A, KVLAT), 1.0, 6.0, ((0, 32),))
    rope_key = draw_rope_key(jax.random.fold_in(keys[17], 71), 0)
    q_gain = jnp.clip(1.0 + 0.18 * jax.random.normal(keys[3], (QLAT,), jnp.float32), 0.099609375, 1.8984375).astype(jnp.bfloat16)
    kv_gain = jnp.clip(1.0 + 0.18 * jax.random.normal(keys[4], (KVLAT,), jnp.float32), 0.099609375, 1.8984375).astype(jnp.bfloat16)
    w_q_nope = centred(keys[5], (QLAT, HEADS * NOPE), QLAT ** -0.5, 0.25, ((1, 16),))
    w_q_rope = centred(keys[6], (QLAT, HEADS * ROPE), QLAT ** -0.5, 0.25, ((1, 16),))
    w_k_nope = centred(keys[7], (KVLAT, HEADS * NOPE), KVLAT ** -0.5, 0.375, ((1, 16),))
    w_value = centred(keys[8], (KVLAT, HEADS * VDIM), KVLAT ** -0.5, 0.375, ((1, 16),))
    w_out = centred(keys[9], (HEADS * VDIM, D), 0.9, 5.375, ((0, 16),))
    tokens_b = centred(keys[10], (TOK_B, D), 1.0, 6.0, ((0, 32),))
    norm_gain_b = jnp.clip(1.0 + 0.18 * jax.random.normal(keys[11], (D,), jnp.float32), 0.099609375, 1.8984375).astype(jnp.bfloat16)
    routes_keys = jax.random.split(jax.random.fold_in(keys[12], 1), TOK_B // R_B)
    routes_turns = jax.random.permutation(jax.random.fold_in(keys[12], 3), TOK_B // R_B)
    routes = jax.vmap(lambda own, number: assign_block(jax.random.fold_in(keys[12], 2), own, number, R_B, EXPERTS, 2, CAP, 2))(routes_keys, routes_turns).reshape((TOK_B, 2))
    route_logits = centred(keys[13], (TOK_B, 2), 1.5, 6.0, ((0, 32),), jnp.float32)
    w_gate = centred(keys[14], (EXPERTS, D, FFE), D ** -0.5, 0.125, ((0, 32), (2, 16)))
    w_up = centred(keys[15], (EXPERTS, D, FFE), D ** -0.5, 0.125, ((0, 32), (2, 16)))
    w_down = noise_with(keys[16], (EXPERTS, FFE, D), FFE ** -0.5, 0.125, ((0, 32), (1, 16)), (1, 2, 16, 2.0))
    return dict(q_latent=q_latent, kv_latent=kv_latent, rope_key=rope_key, q_gain=q_gain, kv_gain=kv_gain, w_q_nope=w_q_nope, w_q_rope=w_q_rope, w_k_nope=w_k_nope, w_value=w_value, w_out=w_out, tokens_b=tokens_b, norm_gain_b=norm_gain_b, routes=routes, route_logits=route_logits, w_gate=w_gate, w_up=w_up, w_down=w_down)


EPSILON = 1e-06

def rms_rows(values, gain):
    wide = values.astype(jnp.float32)
    scaled = wide * lax.rsqrt(lax.optimization_barrier(jnp.mean(wide * wide, axis=-1, keepdims=True)) + EPSILON)
    return (scaled * gain.astype(jnp.float32)).astype(jnp.bfloat16)

def rotate(values, places):
    half = values.shape[-1] // 2
    freqs = 10000.0 ** (-jnp.arange(half, dtype=jnp.float32) / half)
    angles = places.astype(jnp.float32)[:, None] * freqs[None, :]
    cosine = jnp.cos(angles)[:, None, :]
    sine = jnp.sin(angles)[:, None, :]
    first = values[..., :half]
    second = values[..., half:]
    return jnp.concatenate([first * cosine - second * sine, first * sine + second * cosine], axis=-1)

def add_group(acc, operands):
    part = jnp.dot(operands[0], operands[1], preferred_element_type=jnp.float32).astype(jnp.bfloat16)
    part = lax.optimization_barrier(part)
    return (acc + part.astype(jnp.float32), None)

def reference(q_latent, kv_latent, rope_key, q_gain, kv_gain, w_q_nope, w_q_rope, w_k_nope, w_value, w_out, tokens_b, norm_gain_b, routes, route_logits, w_gate, w_up, w_down):
    total = q_latent.shape[0]
    places = jnp.arange(total, dtype=jnp.int32)
    q_normed = rms_rows(q_latent, q_gain)
    q_nope = jnp.dot(q_normed, w_q_nope, preferred_element_type=jnp.float32).astype(jnp.bfloat16)
    q_nope = q_nope.reshape(total, HEADS, NOPE)
    q_turn = jnp.dot(q_normed, w_q_rope, preferred_element_type=jnp.float32).reshape(total, HEADS, ROPE)
    q_rope = rotate(q_turn, places).astype(jnp.bfloat16)
    kv_normed = rms_rows(kv_latent, kv_gain)
    k_nope = jnp.dot(kv_normed, w_k_nope, preferred_element_type=jnp.float32).astype(jnp.bfloat16)
    k_nope = k_nope.reshape(total, HEADS, NOPE)
    values = jnp.dot(kv_normed, w_value, preferred_element_type=jnp.float32).astype(jnp.bfloat16)
    values = values.reshape(total, HEADS, VDIM)
    k_rope = rotate(rope_key.astype(jnp.float32)[:, None, :], places)[:, 0].astype(jnp.bfloat16)
    scale = (NOPE + ROPE) ** (-0.5)

    def one_head(operands):
        head_q, head_r, head_k, head_v = operands
        scores = jnp.dot(head_q, head_k.T, preferred_element_type=jnp.float32)
        scores = (scores + jnp.dot(head_r, k_rope.T, preferred_element_type=jnp.float32)) * scale
        top = lax.optimization_barrier(jnp.max(scores, axis=-1, keepdims=True))
        weights = jnp.exp(scores - top)
        total_w = lax.optimization_barrier(jnp.sum(weights, axis=-1, keepdims=True))
        mixed = jnp.dot(weights.astype(jnp.bfloat16), head_v, preferred_element_type=jnp.float32) / total_w
        return mixed.astype(jnp.bfloat16)
    heads_out = lax.map(one_head, (q_nope.transpose(1, 0, 2), q_rope.transpose(1, 0, 2), k_nope.transpose(1, 0, 2), values.transpose(1, 0, 2)))
    group = HEADS // N_TP
    grouped = heads_out.reshape(N_TP, group, total, VDIM).transpose(0, 2, 1, 3).reshape(N_TP, total, group * VDIM)
    out_rows = w_out.reshape(N_TP, group * VDIM, D)
    summed, _ = lax.scan(add_group, jnp.zeros((total, D), jnp.float32), (grouped, out_rows))
    mixer_out = summed.astype(jnp.bfloat16)
    rows_b = tokens_b.shape[0]
    normed_b = rms_rows(tokens_b, norm_gain_b)
    weights_b = jax.nn.softmax(route_logits.astype(jnp.float32), axis=-1)
    flat = routes.reshape(-1).astype(jnp.int32)
    assigned = flat.shape[0]
    onehot = (flat[:, None] == jnp.arange(EXPERTS, dtype=jnp.int32)[None, :]).astype(jnp.int32)
    slot = lax.optimization_barrier(jnp.sum((jnp.cumsum(onehot, axis=0) - 1) * onehot, axis=1)).astype(jnp.int32)
    room = N_EP * CAP
    table = jnp.full((EXPERTS, room), assigned, jnp.int32).at[flat, slot].set(jnp.arange(assigned, dtype=jnp.int32))
    padded = jnp.concatenate([normed_b, jnp.zeros((1, D), jnp.bfloat16)], axis=0)
    slices = FFE // N_TP

    def one_expert(operands):
        picks, gate_w, up_w, down_w = operands
        rows = padded[picks // 2]
        gate = jnp.dot(rows, gate_w, preferred_element_type=jnp.float32)
        up = jnp.dot(rows, up_w, preferred_element_type=jnp.float32)
        hidden = (jax.nn.silu(gate) * up).astype(jnp.bfloat16)
        hidden = hidden.reshape(room, N_TP, slices).transpose(1, 0, 2)
        down = down_w.reshape(N_TP, slices, D)
        total_e, _ = lax.scan(add_group, jnp.zeros((room, D), jnp.float32), (hidden, down))
        return total_e.astype(jnp.bfloat16)
    expert_out = lax.map(one_expert, (table, w_gate, w_up, w_down)).reshape(EXPERTS * room, D)
    where = (flat * room + slot).reshape(rows_b, 2)
    picked = expert_out[where].astype(jnp.float32)
    expert_mix = lax.optimization_barrier(jnp.sum(picked * weights_b[:, :, None], axis=1)).astype(jnp.bfloat16)
    return (mixer_out, expert_mix)
```

```python
import math

import jax
import jax.numpy as jnp
from jax import lax
from jax.experimental import pallas as pl
from jax.experimental.pallas import tpu as pltpu
from jax.sharding import Mesh, PartitionSpec as P


NOPE = 64
ROPE = 32
VDIM = 64
EPSILON = 1e-06
EP = ("z", "c")
TP = ("y", "x")
F32 = jnp.float32
BF16 = jnp.bfloat16
MIB = 1 << 20


def params(mib):
    return pltpu.CompilerParams(vmem_limit_bytes=mib * MIB)


def turns(places, half):
    freqs = 10000.0 ** (-jnp.arange(half, dtype=F32) / half)
    angles = freqs[:, None] * places.astype(F32)[None, :]
    return jnp.cos(angles), jnp.sin(angles)


def dispatch_kernel(experts, room, at_ref, tokens_ref, gain_ref, routes_ref, out_ref, where_ref):
    rows, width = tokens_ref.shape
    share, pitch = out_ref.shape[2], 16 * (-(-room // 16))
    wide = tokens_ref[...].astype(F32)
    mean = jnp.sum(wide * wide, axis=-1, keepdims=True) * (1.0 / width)
    start = pl.multiple_of(at_ref[0] * share, share)
    mine = tokens_ref[:, pl.ds(start, share)].astype(F32) * lax.rsqrt(mean + EPSILON)
    normed = (mine * gain_ref[:, pl.ds(start, share)].astype(F32)).astype(BF16)
    names = lax.broadcasted_iota(jnp.int32, (experts, rows), 0)
    first, second = routes_ref[0:1, :], routes_ref[1:2, :]
    hit_first = jnp.where(names == first, 1.0, 0.0)
    hit_second = jnp.where(names == second, 1.0, 0.0)
    before = lax.broadcasted_iota(jnp.int32, (rows, rows), 0) < lax.broadcasted_iota(
        jnp.int32, (rows, rows), 1
    )
    earlier = jnp.where(before, 1.0, 0.0).astype(BF16)
    seen = jnp.dot((hit_first + hit_second).astype(BF16), earlier, preferred_element_type=F32)
    slot_first = jnp.sum(seen * hit_first, axis=0, keepdims=True)
    slot_second = jnp.sum(seen * hit_second, axis=0, keepdims=True)
    to_first = first * pitch + slot_first.astype(jnp.int32)
    to_second = second * pitch + slot_second.astype(jnp.int32)
    where_ref[0:1, :] = to_first
    where_ref[1:2, :] = to_second
    places = lax.broadcasted_iota(jnp.int32, (experts * pitch, rows), 0)
    chosen = jnp.where((places == to_first) | (places == to_second), 1.0, 0.0).astype(BF16)
    picked = jnp.dot(chosen, normed, preferred_element_type=F32).astype(BF16)
    out_ref[...] = picked.reshape(experts, pitch, share)[:, :room]


def dispatch(tokens, gain, routes, at, experts, room, share):
    rows = tokens.shape[0]
    vmem = pl.BlockSpec(memory_space=pltpu.VMEM)
    return pl.pallas_call(
        lambda *refs: dispatch_kernel(experts, room, *refs),
        out_shape=(
            jax.ShapeDtypeStruct((experts, room, share), BF16),
            jax.ShapeDtypeStruct((2, rows), jnp.int32),
        ),
        in_specs=[pl.BlockSpec(memory_space=pltpu.SMEM), vmem, vmem, vmem],
        out_specs=(vmem, vmem),
        compiler_params=params(60),
        cost_estimate=pl.CostEstimate(flops=10_000_000, bytes_accessed=700_000, transcendentals=0),
        name="dispatch",
    )(at, tokens, gain.reshape(1, -1), routes.T)


def expert_kernel(x_ref, gate_hbm, up_hbm, down_hbm, out_ref, gate_ref, up_ref, down_ref, sems):
    pieces, rows, share = x_ref.shape
    loads = [
        pltpu.make_async_copy(source, target, sems.at[n])
        for n, (source, target) in enumerate(
            ((gate_hbm, gate_ref), (up_hbm, up_ref), (down_hbm, down_ref))
        )
    ]
    for load in loads:
        load.start()
    loads[0].wait()
    loads[1].wait()
    step = 128
    for at in range(0, rows, step):
        x = jnp.concatenate([x_ref[p, at : at + step, :] for p in range(pieces)], axis=1)
        gate = jnp.dot(x, gate_ref[...], preferred_element_type=F32)
        up = jnp.dot(x, up_ref[...], preferred_element_type=F32)
        hidden = (gate / (1.0 + jnp.exp(-gate)) * up).astype(BF16)
        if at == 0:
            loads[2].wait()
        for p in range(0, pieces, 2):
            term = jnp.dot(
                hidden, down_ref[:, p * share : (p + 2) * share], preferred_element_type=F32
            ).astype(BF16)
            out_ref[p, at : at + step, :] = term[:, :share]
            out_ref[p + 1, at : at + step, :] = term[:, share:]


def expert(x, gate, up, down):
    vmem = pl.BlockSpec(memory_space=pltpu.VMEM)
    return pl.pallas_call(
        expert_kernel,
        out_shape=jax.ShapeDtypeStruct(x.shape, BF16),
        in_specs=[vmem] + [pl.BlockSpec(memory_space=pl.ANY)] * 3,
        out_specs=vmem,
        scratch_shapes=[pltpu.VMEM(w.shape, BF16) for w in (gate, up, down)]
        + [pltpu.SemaphoreType.DMA((3,))],
        compiler_params=params(56),
        cost_estimate=pl.CostEstimate(flops=40_000_000, bytes_accessed=6_000_000, transcendentals=0),
        name="expert",
    )(x, gate, up, down)


def combine_kernel(back_ref, where_ref, logits_ref, out_ref, wide_ref):
    rows, share = out_ref.shape
    wide_ref[...] = jnp.zeros_like(wide_ref)
    wide_ref[:, : back_ref.shape[1]] = back_ref[...]
    back = wide_ref[...].reshape(-1, share)
    places = lax.broadcasted_iota(jnp.int32, (rows, back.shape[0]), 1)
    left, right = logits_ref[:, 0:1], logits_ref[:, 1:2]
    top = jnp.maximum(left, right)
    grow_left, grow_right = jnp.exp(left - top), jnp.exp(right - top)
    both = grow_left + grow_right
    mixed = jnp.zeros(out_ref.shape, F32)
    for k, grown in ((0, grow_left), (1, grow_right)):
        chosen = jnp.where(places == where_ref[:, k : k + 1], 1.0, 0.0).astype(BF16)
        picked = jnp.dot(chosen, back, preferred_element_type=F32)
        mixed = mixed + picked * (grown / both)
    out_ref[...] = mixed.astype(BF16)


def combine(back, where, logits):
    vmem = pl.BlockSpec(memory_space=pltpu.VMEM)
    return pl.pallas_call(
        combine_kernel,
        out_shape=jax.ShapeDtypeStruct((logits.shape[0], back.shape[2]), BF16),
        in_specs=[vmem] * 3,
        out_specs=vmem,
        scratch_shapes=[pltpu.VMEM((back.shape[0], 16 * (-(-back.shape[1] // 16)), back.shape[2]), BF16)],
        compiler_params=params(8),
        name="combine",
    )(back, where, logits)


def normed_rows(ref, gain_ref):
    wide = ref[...].astype(F32)
    mean = jnp.sum(wide * wide, axis=-1, keepdims=True) * (1.0 / ref.shape[1])
    return (wide * lax.rsqrt(mean + EPSILON) * gain_ref[...].astype(F32)).astype(BF16)


def across(left, right):
    return lax.dot_general(left, right, (((1,), (1,)), ((), ())), preferred_element_type=F32)


def turned(values, cosine, sine):
    half = values.shape[0] // 2
    first, second = values[:half], values[half:]
    return first * cosine - second * sine, first * sine + second * cosine


def keys_kernel(kv_ref, gain_ref, rope_ref, key_ref, value_ref, cos_ref, sin_ref, out_ref):
    normed = normed_rows(kv_ref, gain_ref)
    half = ROPE // 2
    first, second = turned(rope_ref[...].astype(F32), cos_ref[...], sin_ref[...])
    out_ref[:NOPE] = across(key_ref[...], normed).astype(BF16)
    out_ref[NOPE : NOPE + half] = first.astype(BF16)
    out_ref[NOPE + half : NOPE + ROPE] = second.astype(BF16)
    out_ref[NOPE + ROPE :] = across(value_ref[...], normed).astype(BF16)


def keys(kv, gain, rope_key, w_key, w_value, cosine, sine):
    vmem = pl.BlockSpec(memory_space=pltpu.VMEM)
    return pl.pallas_call(
        keys_kernel,
        out_shape=jax.ShapeDtypeStruct((NOPE + ROPE + VDIM, kv.shape[0]), BF16),
        in_specs=[vmem] * 7,
        out_specs=vmem,
        compiler_params=params(60),
        cost_estimate=pl.CostEstimate(flops=10_000_000, bytes_accessed=500_000, transcendentals=0),
        name="keys",
    )(kv, gain.reshape(1, -1), rope_key.T, w_key.T, w_value.T, cosine, sine)


def queries_kernel(side, q_ref, gain_ref, nope_ref, rope_ref, cos_ref, sin_ref, out_ref):
    normed = normed_rows(q_ref, gain_ref)
    rows = normed.shape[0]
    few = rows // (side * side)
    order = [(y * side + x) * few for x in range(side) for y in range(side)]
    normed = jnp.concatenate([normed[at : at + few] for at in order], axis=0)
    half = ROPE // 2
    out_ref[:NOPE] = across(nope_ref[...], normed).astype(BF16)
    first, second = turned(across(rope_ref[...], normed), cos_ref[...], sin_ref[...])
    out_ref[NOPE : NOPE + half] = first.astype(BF16)
    out_ref[NOPE + half : NOPE + ROPE] = second.astype(BF16)
    out_ref[NOPE + ROPE :] = jnp.zeros((out_ref.shape[0] - NOPE - ROPE, rows), BF16)


def queries(q_latent, gain, w_nope, w_rope, cosine, sine, side):
    vmem = pl.BlockSpec(memory_space=pltpu.VMEM)
    return pl.pallas_call(
        lambda *refs: queries_kernel(side, *refs),
        out_shape=jax.ShapeDtypeStruct((128, q_latent.shape[0]), BF16),
        in_specs=[vmem] * 6,
        out_specs=vmem,
        compiler_params=params(60),
        cost_estimate=pl.CostEstimate(flops=10_000_000, bytes_accessed=700_000, transcendentals=0),
        name="queries",
    )(q_latent, gain.reshape(1, -1), w_nope.T, w_rope.T, cosine, sine)


def attention_kernel(q_ref, own_ref, other_ref, out_ref, s_ref, acc_ref):
    tile = 256
    blocks, _, span = own_ref.shape
    queries = q_ref.shape[1]
    cut = NOPE + ROPE
    rate = (NOPE + ROPE) ** (-0.5) * math.log2(math.e)
    pad = jnp.zeros((q_ref.shape[0] - cut, tile), BF16)
    ones = jnp.ones((16, tile), BF16)
    tiles = [(ref, at) for ref in (own_ref, other_ref) for at in range(0, span, tile)]
    halves = range(0, queries, tile)

    def score(block, slot, top):
        tops = [None for _ in halves]
        for n, (ref, at) in enumerate(tiles):
            keys = jnp.concatenate([ref[block, :cut, at : at + tile], pad], axis=0).T
            for i, h in enumerate(halves):
                s = jnp.dot(keys, q_ref[:, h : h + tile], preferred_element_type=F32)
                s_ref[slot, n * tile : (n + 1) * tile, h : h + tile] = s
                most = jnp.max(s.reshape(tile // 8, 8, tile), axis=0)
                tops[i] = most if tops[i] is None else jnp.maximum(tops[i], most)
        block_top = jnp.max(jnp.concatenate(tops, axis=1), axis=0, keepdims=True)
        return jnp.maximum(top, block_top)

    def absorb(block, slot, old_top, top):
        shrink = jnp.exp2((old_top - top) * rate)
        for h in halves:
            total = acc_ref[:, h : h + tile] * shrink[:, h : h + tile]
            for n, (ref, at) in enumerate(tiles):
                s = s_ref[slot, n * tile : (n + 1) * tile, h : h + tile]
                weights = jnp.exp2((s - top[:, h : h + tile]) * rate).astype(BF16)
                rows = jnp.concatenate([ref[block, cut:, at : at + tile], ones], axis=0)
                total = total + jnp.dot(rows, weights, preferred_element_type=F32)
            acc_ref[:, h : h + tile] = total

    def pair(turn, carry):
        old_top, top = carry
        for slot in (0, 1):
            block = turn * 2 + slot
            ahead = jnp.minimum(block + 1, blocks - 1)
            new_top = score(ahead, 1 - slot, top)
            absorb(block, slot, old_top, top)
            old_top, top = top, new_top
        return old_top, top

    acc_ref[...] = jnp.zeros_like(acc_ref)
    floor = jnp.full((1, queries), -1e30, F32)
    lax.fori_loop(0, blocks // 2, pair, (floor, score(0, 0, floor)))

    done = (acc_ref[:VDIM, :] / acc_ref[VDIM : VDIM + 1, :]).astype(BF16)
    for n in range(out_ref.shape[0]):
        out_ref[n] = done[:, n * out_ref.shape[2] : (n + 1) * out_ref.shape[2]]


def attention(q, own, other, parts):
    vmem = pl.BlockSpec(memory_space=pltpu.VMEM)
    queries = q.shape[1]
    return pl.pallas_call(
        attention_kernel,
        out_shape=jax.ShapeDtypeStruct((parts, VDIM, queries // parts), BF16),
        in_specs=[vmem] * 3,
        out_specs=vmem,
        scratch_shapes=[
            pltpu.VMEM((2, 2 * own.shape[2], queries), F32),
            pltpu.VMEM((VDIM + 16, queries), F32),
        ],
        compiler_params=params(24),
        cost_estimate=pl.CostEstimate(flops=200_000_000, bytes_accessed=8_000_000, transcendentals=0),
        name="attention",
    )(q, own, other)


def ring(count, step):
    return [(i, (i + step) % count) for i in range(count)]


def from_row(value, axis):
    count = lax.axis_size(axis)
    return [value] + [lax.ppermute(value, axis, ring(count, k)) for k in range(1, count)]


def traded(pieces, axis):
    count, me = lax.axis_size(axis), lax.axis_index(axis)
    mine = lambda k: lax.dynamic_index_in_dim(pieces, lax.rem(me + k, count), 0, False, allow_negative_indices=False)
    return [mine(0)] + [
        lax.ppermute(mine(k), axis, ring(count, k)) for k in range(1, count)
    ]


def shards(
    q_latent,
    kv_latent,
    rope_key,
    q_gain,
    kv_gain,
    w_q_nope,
    w_q_rope,
    w_k_nope,
    w_value,
    w_out,
    tokens_b,
    norm_gain_b,
    routes,
    route_logits,
    w_gate,
    w_up,
    w_down,
):
    n_ep, n_tp = lax.axis_size(EP), lax.axis_size(TP)
    side = lax.axis_size("x")
    rows_b, width = tokens_b.shape
    room = 3 * rows_b // n_ep
    share = width // n_tp
    own_rows = q_latent.shape[0]
    first_row = lax.axis_index(EP) * own_rows
    places = jnp.arange(own_rows, dtype=jnp.int32)
    cos_k, sin_k = turns(first_row + places, ROPE // 2)
    mixed = places.reshape(side, side, -1).transpose(1, 0, 2).reshape(-1)
    cos_q, sin_q = turns(first_row + mixed, ROPE // 2)
    piece = keys(kv_latent, kv_gain, rope_key, w_k_nope, w_value, cos_k, sin_k)
    own = lax.all_gather(piece, "z", axis=0, tiled=False)
    routes, piece = lax.optimization_barrier((routes, piece))
    outgoing, where = dispatch(
        tokens_b, norm_gain_b, routes, lax.axis_index(TP)[None], n_ep, room, share
    )
    arrived = lax.all_to_all(outgoing, EP, split_axis=0, concat_axis=0, tiled=True)
    w_group = jnp.concatenate(from_row(w_out, "x"), axis=0)
    q = queries(q_latent, q_gain, w_q_nope, w_q_rope, cos_q, sin_q, side)
    mine = arrived.reshape(1, n_ep * room, share)
    mine = jnp.broadcast_to(mine, (n_tp, n_ep * room, share))
    rows = lax.all_to_all(mine, TP, split_axis=0, concat_axis=0, tiled=True)
    terms = expert(rows, w_gate[0], w_up[0], w_down[0])
    terms = lax.all_to_all(terms, TP, split_axis=0, concat_axis=0, tiled=True)
    other = lax.ppermute(own, "c", [(0, 1), (1, 0)])
    heads = attention(q, own, other, side)
    heads = jnp.concatenate(traded(heads, "x"), axis=0)
    partial = lax.dot_general(
        heads, w_group, (((0,), (0,)), ((), ())), preferred_element_type=F32
    ).astype(BF16)
    partial = partial.reshape(side, own_rows // n_tp, width)
    partial = traded(partial, "y")
    finished = terms.astype(F32).sum(axis=0).astype(BF16)
    back = lax.all_to_all(
        finished.reshape(n_ep, room, share), EP, split_axis=0, concat_axis=0, tiled=True
    )
    expert_mix = combine(back, where.T, route_logits)
    mixer_out = sum(p.astype(F32) for p in partial).astype(BF16)
    return (mixer_out, expert_mix)


def solution(mesh):
    n_ep, n_tp = mesh.shape["ep"], mesh.shape["tp"]
    side = math.isqrt(n_tp)
    split = Mesh(
        mesh.devices.reshape(n_ep // 2, 2, side, n_tp // side), ("z", "c", "y", "x")
    )
    placed = (
        P(EP, None),
        P(EP, None),
        P(EP, None),
        P(),
        P(),
        P(None, TP),
        P(None, TP),
        P(None, TP),
        P(None, TP),
        P(TP, None),
        P(EP, None),
        P(),
        P(EP, None),
        P(EP, None),
        P(EP, None, TP),
        P(EP, None, TP),
        P(EP, TP, None),
    )
    return jax.shard_map(
        shards,
        mesh=split,
        in_specs=placed,
        out_specs=(P(EP + TP, None), P(EP, TP)),
        check_vma=False,
    )
```

```python
import math

import jax
import jax.numpy as jnp
from jax import lax
from jax.experimental import pallas as pl
from jax.experimental.pallas import tpu as pltpu
from jax.sharding import Mesh, PartitionSpec as P


NOPE = 64
ROPE = 32
VDIM = 64
EPSILON = 1e-06
EP = ("z", "c")
TP = ("y", "x")
F32 = jnp.float32
BF16 = jnp.bfloat16
MIB = 1 << 20


def params(mib):
    return pltpu.CompilerParams(vmem_limit_bytes=mib * MIB)


def turns(places, half):
    freqs = 10000.0 ** (-jnp.arange(half, dtype=F32) / half)
    angles = freqs[:, None] * places.astype(F32)[None, :]
    return jnp.cos(angles), jnp.sin(angles)


def dispatch_kernel(
    experts, room, at_ref, tokens_ref, gain_ref, routes_ref, out_ref, where_ref, row_ref
):
    rows, width = tokens_ref.shape
    share, pitch = out_ref.shape[2], 16 * (-(-room // 16))
    wide = tokens_ref[...].astype(F32)
    mean = jnp.sum(wide * wide, axis=-1, keepdims=True) * (1.0 / width)
    start = pl.multiple_of(at_ref[0] * share, share)
    row_ref[...] = gain_ref[...].astype(F32)[None, :]
    mine = tokens_ref[:, pl.ds(start, share)].astype(F32) * lax.rsqrt(mean + EPSILON)
    normed = (mine * row_ref[:, pl.ds(start, share)]).astype(BF16)
    names = lax.broadcasted_iota(jnp.int32, (experts, rows), 0)
    first, second = routes_ref[0:1, :], routes_ref[1:2, :]
    hit_first = jnp.where(names == first, 1.0, 0.0)
    hit_second = jnp.where(names == second, 1.0, 0.0)
    before = lax.broadcasted_iota(jnp.int32, (rows, rows), 0) < lax.broadcasted_iota(
        jnp.int32, (rows, rows), 1
    )
    earlier = jnp.where(before, 1.0, 0.0).astype(BF16)
    seen = jnp.dot((hit_first + hit_second).astype(BF16), earlier, preferred_element_type=F32)
    slot_first = jnp.sum(seen * hit_first, axis=0, keepdims=True)
    slot_second = jnp.sum(seen * hit_second, axis=0, keepdims=True)
    to_first = first * pitch + slot_first.astype(jnp.int32)
    to_second = second * pitch + slot_second.astype(jnp.int32)
    where_ref[0:1, :] = to_first
    where_ref[1:2, :] = to_second
    places = lax.broadcasted_iota(jnp.int32, (experts * pitch, rows), 0)
    chosen = jnp.where((places == to_first) | (places == to_second), 1.0, 0.0).astype(BF16)
    picked = jnp.dot(chosen, normed, preferred_element_type=F32).astype(BF16)
    out_ref[...] = picked.reshape(experts, pitch, share)[:, :room]


def dispatch(tokens, gain, routes, at, experts, room, share):
    rows = tokens.shape[0]
    vmem = pl.BlockSpec(memory_space=pltpu.VMEM)
    return pl.pallas_call(
        lambda *refs: dispatch_kernel(experts, room, *refs),
        out_shape=(
            jax.ShapeDtypeStruct((experts, room, share), BF16),
            jax.ShapeDtypeStruct((2, rows), jnp.int32),
        ),
        in_specs=[pl.BlockSpec(memory_space=pltpu.SMEM), vmem, vmem, vmem],
        out_specs=(vmem, vmem),
        scratch_shapes=[pltpu.VMEM((1, tokens.shape[1]), F32)],
        compiler_params=params(60),
        cost_estimate=pl.CostEstimate(flops=10_000_000, bytes_accessed=700_000, transcendentals=0),
        name="dispatch",
    )(at, tokens, gain, routes.T)


def expert_kernel(x_hbm, gate_hbm, up_hbm, down_hbm, out_ref, x_ref, gate_ref, up_ref, down_ref, gate_acc, up_acc, sems):
    pieces, rows, share = x_ref.shape
    step, few = 128, pieces // 4
    loads = []
    for n in range(4):
        some, deep = pl.ds(n * few, few), pl.ds(n * few * share, few * share)
        for m, (source, target, part) in enumerate(
            ((x_hbm, x_ref, some), (gate_hbm, gate_ref, deep), (up_hbm, up_ref, deep))
        ):
            loads.append(
                pltpu.make_async_copy(source.at[part], target.at[part], sems.at[3 * n + m])
            )
    loads.append(pltpu.make_async_copy(down_hbm, down_ref, sems.at[12]))
    for load in loads:
        load.start()
    for n in range(4):
        for load in loads[3 * n : 3 * n + 3]:
            load.wait()
        deep = pl.ds(n * few * share, few * share)
        for at in range(0, rows, step):
            x = jnp.concatenate(
                [x_ref[n * few + p, at : at + step, :] for p in range(few)], axis=1
            )
            gate = jnp.dot(x, gate_ref[deep, :], preferred_element_type=F32)
            up = jnp.dot(x, up_ref[deep, :], preferred_element_type=F32)
            if n:
                gate = gate + gate_acc[at : at + step, :]
                up = up + up_acc[at : at + step, :]
            gate_acc[at : at + step, :] = gate
            up_acc[at : at + step, :] = up
    loads[12].wait()
    for at in range(0, rows, step):
        gate, up = gate_acc[at : at + step, :], up_acc[at : at + step, :]
        hidden = (gate / (1.0 + jnp.exp(-gate)) * up).astype(BF16)
        for p in range(0, pieces, 2):
            term = jnp.dot(
                hidden, down_ref[:, p * share : (p + 2) * share], preferred_element_type=F32
            ).astype(BF16)
            out_ref[p, at : at + step, :] = term[:, :share]
            out_ref[p + 1, at : at + step, :] = term[:, share:]


def expert(x, gate, up, down):
    anywhere = pl.BlockSpec(memory_space=pl.ANY)
    return pl.pallas_call(
        expert_kernel,
        out_shape=jax.ShapeDtypeStruct(x.shape, BF16),
        in_specs=[anywhere] * 4,
        out_specs=pl.BlockSpec(memory_space=pltpu.VMEM),
        scratch_shapes=[pltpu.VMEM(w.shape, BF16) for w in (x, gate, up, down)]
        + [pltpu.VMEM((x.shape[1], gate.shape[1]), F32)] * 2
        + [pltpu.SemaphoreType.DMA((13,))],
        compiler_params=params(60),
        cost_estimate=pl.CostEstimate(flops=40_000_000, bytes_accessed=6_000_000, transcendentals=0),
        name="expert",
    )(x, gate, up, down)


def combine_kernel(back_ref, where_ref, logits_ref, out_ref, wide_ref):
    rows, share = out_ref.shape
    wide_ref[...] = jnp.zeros_like(wide_ref)
    wide_ref[:, : back_ref.shape[1]] = back_ref[...]
    back = wide_ref[...].reshape(-1, share)
    places = lax.broadcasted_iota(jnp.int32, (rows, back.shape[0]), 1)
    left, right = logits_ref[:, 0:1], logits_ref[:, 1:2]
    top = jnp.maximum(left, right)
    grow_left, grow_right = jnp.exp(left - top), jnp.exp(right - top)
    both = grow_left + grow_right
    mixed = jnp.zeros(out_ref.shape, F32)
    for k, grown in ((0, grow_left), (1, grow_right)):
        chosen = jnp.where(places == where_ref[:, k : k + 1], 1.0, 0.0).astype(BF16)
        picked = jnp.dot(chosen, back, preferred_element_type=F32)
        mixed = mixed + picked * (grown / both)
    out_ref[...] = mixed.astype(BF16)


def combine(back, where, logits):
    vmem = pl.BlockSpec(memory_space=pltpu.VMEM)
    return pl.pallas_call(
        combine_kernel,
        out_shape=jax.ShapeDtypeStruct((logits.shape[0], back.shape[2]), BF16),
        in_specs=[vmem] * 3,
        out_specs=vmem,
        scratch_shapes=[pltpu.VMEM((back.shape[0], 16 * (-(-back.shape[1] // 16)), back.shape[2]), BF16)],
        compiler_params=params(8),
        name="combine",
    )(back, where, logits)


def normed_rows(ref, gain_ref):
    wide = ref[...].astype(F32)
    mean = jnp.sum(wide * wide, axis=-1, keepdims=True) * (1.0 / ref.shape[1])
    return (wide * lax.rsqrt(mean + EPSILON) * gain_ref[...].astype(F32)[None, :]).astype(BF16)


def across(left, right):
    return lax.dot_general(left, right, (((1,), (1,)), ((), ())), preferred_element_type=F32)


def turned(values, cosine, sine):
    half = values.shape[0] // 2
    first, second = values[:half], values[half:]
    return first * cosine - second * sine, first * sine + second * cosine


def keys_kernel(kv_ref, gain_ref, rope_ref, key_ref, value_ref, cos_ref, sin_ref, out_ref):
    normed = normed_rows(kv_ref, gain_ref)
    half = ROPE // 2
    first, second = turned(rope_ref[...].astype(F32), cos_ref[...], sin_ref[...])
    out_ref[:NOPE] = across(key_ref[...], normed).astype(BF16)
    out_ref[NOPE : NOPE + half] = first.astype(BF16)
    out_ref[NOPE + half : NOPE + ROPE] = second.astype(BF16)
    out_ref[NOPE + ROPE :] = across(value_ref[...], normed).astype(BF16)


def keys(kv, gain, rope_key, w_key, w_value, cosine, sine):
    vmem = pl.BlockSpec(memory_space=pltpu.VMEM)
    return pl.pallas_call(
        keys_kernel,
        out_shape=jax.ShapeDtypeStruct((NOPE + ROPE + VDIM, kv.shape[0]), BF16),
        in_specs=[vmem] * 7,
        out_specs=vmem,
        compiler_params=params(60),
        cost_estimate=pl.CostEstimate(flops=10_000_000, bytes_accessed=500_000, transcendentals=0),
        name="keys",
    )(kv, gain, rope_key.T, w_key.T, w_value.T, cosine, sine)


def queries_kernel(side, q_ref, gain_ref, nope_ref, rope_ref, cos_ref, sin_ref, out_ref):
    normed = normed_rows(q_ref, gain_ref)
    rows = normed.shape[0]
    few = rows // (side * side)
    order = [(y * side + x) * few for x in range(side) for y in range(side)]
    normed = jnp.concatenate([normed[at : at + few] for at in order], axis=0)
    half = ROPE // 2
    out_ref[:NOPE] = across(nope_ref[...], normed).astype(BF16)
    first, second = turned(across(rope_ref[...], normed), cos_ref[...], sin_ref[...])
    out_ref[NOPE : NOPE + half] = first.astype(BF16)
    out_ref[NOPE + half : NOPE + ROPE] = second.astype(BF16)
    out_ref[NOPE + ROPE :] = jnp.zeros((out_ref.shape[0] - NOPE - ROPE, rows), BF16)


def queries(q_latent, gain, w_nope, w_rope, cosine, sine, side):
    vmem = pl.BlockSpec(memory_space=pltpu.VMEM)
    return pl.pallas_call(
        lambda *refs: queries_kernel(side, *refs),
        out_shape=jax.ShapeDtypeStruct((128, q_latent.shape[0]), BF16),
        in_specs=[vmem] * 6,
        out_specs=vmem,
        compiler_params=params(60),
        cost_estimate=pl.CostEstimate(flops=10_000_000, bytes_accessed=700_000, transcendentals=0),
        name="queries",
    )(q_latent, gain, w_nope.T, w_rope.T, cosine, sine)


def attention_kernel(q_ref, kv_ref, out_ref, s_ref, acc_ref):
    tile = 256
    blocks, span = kv_ref.shape[0] // 2, kv_ref.shape[2]
    queries = q_ref.shape[1]
    cut = NOPE + ROPE
    rate = (NOPE + ROPE) ** (-0.5) * math.log2(math.e)
    pad = jnp.zeros((q_ref.shape[0] - cut, tile), BF16)
    ones = jnp.ones((16, tile), BF16)
    tiles = [(part, at) for part in (0, 1) for at in range(0, span, tile)]
    halves = range(0, queries, tile)

    def score(block, slot, top):
        tops = [None for _ in halves]
        for n, (part, at) in enumerate(tiles):
            keys = jnp.concatenate([kv_ref[2 * block + part, :cut, at : at + tile], pad], axis=0).T
            for i, h in enumerate(halves):
                s = jnp.dot(keys, q_ref[:, h : h + tile], preferred_element_type=F32)
                s_ref[slot, n * tile : (n + 1) * tile, h : h + tile] = s
                most = jnp.max(s.reshape(tile // 8, 8, tile), axis=0)
                tops[i] = most if tops[i] is None else jnp.maximum(tops[i], most)
        block_top = jnp.max(jnp.concatenate(tops, axis=1), axis=0, keepdims=True)
        return jnp.maximum(top, block_top)

    def absorb(block, slot, old_top, top):
        shrink = jnp.exp2((old_top - top) * rate)
        for h in halves:
            total = acc_ref[:, h : h + tile] * shrink[:, h : h + tile]
            for n, (part, at) in enumerate(tiles):
                s = s_ref[slot, n * tile : (n + 1) * tile, h : h + tile]
                weights = jnp.exp2((s - top[:, h : h + tile]) * rate).astype(BF16)
                rows = jnp.concatenate([kv_ref[2 * block + part, cut:, at : at + tile], ones], axis=0)
                total = total + jnp.dot(rows, weights, preferred_element_type=F32)
            acc_ref[:, h : h + tile] = total

    def pair(turn, carry):
        old_top, top = carry
        for slot in (0, 1):
            block = turn * 2 + slot
            ahead = jnp.minimum(block + 1, blocks - 1)
            new_top = score(ahead, 1 - slot, top)
            absorb(block, slot, old_top, top)
            old_top, top = top, new_top
        return old_top, top

    acc_ref[...] = jnp.zeros_like(acc_ref)
    floor = jnp.full((1, queries), -1e30, F32)
    lax.fori_loop(0, blocks // 2, pair, (floor, score(0, 0, floor)))

    done = (acc_ref[:VDIM, :] / acc_ref[VDIM : VDIM + 1, :]).astype(BF16)
    for n in range(out_ref.shape[0]):
        out_ref[n] = done[:, n * out_ref.shape[2] : (n + 1) * out_ref.shape[2]]


def attention(q, kv, parts):
    vmem = pl.BlockSpec(memory_space=pltpu.VMEM)
    queries = q.shape[1]
    return pl.pallas_call(
        attention_kernel,
        out_shape=jax.ShapeDtypeStruct((parts, VDIM, queries // parts), BF16),
        in_specs=[vmem] * 2,
        out_specs=vmem,
        scratch_shapes=[
            pltpu.VMEM((2, 2 * kv.shape[2], queries), F32),
            pltpu.VMEM((VDIM + 16, queries), F32),
        ],
        compiler_params=params(24),
        cost_estimate=pl.CostEstimate(flops=200_000_000, bytes_accessed=8_000_000, transcendentals=0),
        name="attention",
    )(q, kv)


def ring(count, step):
    return [(i, (i + step) % count) for i in range(count)]


def from_row(value, axis):
    count = lax.axis_size(axis)
    return [value] + [lax.ppermute(value, axis, ring(count, k)) for k in range(1, count)]


def traded(pieces, axis):
    count, me = lax.axis_size(axis), lax.axis_index(axis)
    mine = lambda k: lax.dynamic_index_in_dim(pieces, lax.rem(me + k, count), 0, False, allow_negative_indices=False)
    return [mine(0)] + [
        lax.ppermute(mine(k), axis, ring(count, k)) for k in range(1, count)
    ]


def traded_in_two(pieces, axis):
    count, me = lax.axis_size(axis), lax.axis_index(axis)
    doubled = jnp.concatenate([pieces, pieces], axis=0)
    turned_pieces = lax.dynamic_slice_in_dim(doubled, me, count, 0, allow_negative_indices=False)
    far = lax.ppermute(turned_pieces[2:], axis, ring(count, 2))
    near = lax.ppermute(
        jnp.concatenate([turned_pieces[1:2], far[1:]], axis=0), axis, ring(count, 1)
    )
    return [turned_pieces[0], near[0], far[0], near[1]]


def shards(
    q_latent,
    kv_latent,
    rope_key,
    q_gain,
    kv_gain,
    w_q_nope,
    w_q_rope,
    w_k_nope,
    w_value,
    w_out,
    tokens_b,
    norm_gain_b,
    routes,
    route_logits,
    w_gate,
    w_up,
    w_down,
):
    n_ep, n_tp = lax.axis_size(EP), lax.axis_size(TP)
    side = lax.axis_size("x")
    rows_b, width = tokens_b.shape
    room = 3 * rows_b // n_ep
    share = width // n_tp
    own_rows = q_latent.shape[0]
    first_row = lax.axis_index(EP) * own_rows
    places = jnp.arange(own_rows, dtype=jnp.int32)
    cos_k, sin_k = turns(first_row + places, ROPE // 2)
    mixed = places.reshape(side, side, -1).transpose(1, 0, 2).reshape(-1)
    cos_q, sin_q = turns(first_row + mixed, ROPE // 2)
    piece = keys(kv_latent, kv_gain, rope_key, w_k_nope, w_value, cos_k, sin_k)
    gathered = lax.all_gather(piece, EP, axis=0, tiled=False)
    routes, piece = lax.optimization_barrier((routes, piece))
    outgoing, where = dispatch(
        tokens_b, norm_gain_b, routes, lax.axis_index(TP)[None], n_ep, room, share
    )
    arrived = lax.all_to_all(outgoing, EP, split_axis=0, concat_axis=0, tiled=True)
    w_group = jnp.concatenate(from_row(w_out, "x"), axis=0)
    q = queries(q_latent, q_gain, w_q_nope, w_q_rope, cos_q, sin_q, side)
    mine = arrived.reshape(1, n_ep * room, share)
    mine = jnp.broadcast_to(mine, (n_tp, n_ep * room, share))
    rows = lax.all_to_all(mine, TP, split_axis=0, concat_axis=0, tiled=True)
    terms = expert(rows, w_gate[0], w_up[0], w_down[0])
    terms = lax.all_to_all(terms, TP, split_axis=0, concat_axis=0, tiled=True)
    heads = attention(q, gathered, side)
    heads = jnp.concatenate(traded_in_two(heads, "x"), axis=0)
    partial = lax.dot_general(
        heads, w_group, (((0,), (0,)), ((), ())), preferred_element_type=F32
    ).astype(BF16)
    partial = partial.reshape(side, own_rows // n_tp, width)
    partial = traded(partial, "y")
    finished = terms.astype(F32).sum(axis=0).astype(BF16)
    back = lax.all_to_all(
        finished.reshape(n_ep, room, share), EP, split_axis=0, concat_axis=0, tiled=True
    )
    expert_mix = combine(back, where.T, route_logits)
    mixer_out = sum(p.astype(F32) for p in partial).astype(BF16)
    return (mixer_out, expert_mix)


def solution(mesh):
    n_ep, n_tp = mesh.shape["ep"], mesh.shape["tp"]
    side = math.isqrt(n_tp)
    split = Mesh(
        mesh.devices.reshape(n_ep // 2, 2, side, n_tp // side), ("z", "c", "y", "x")
    )
    placed = (
        P(EP, None),
        P(EP, None),
        P(EP, None),
        P(),
        P(),
        P(None, TP),
        P(None, TP),
        P(None, TP),
        P(None, TP),
        P(TP, None),
        P(EP, None),
        P(),
        P(EP, None),
        P(EP, None),
        P(EP, None, TP),
        P(EP, None, TP),
        P(EP, TP, None),
    )
    return jax.shard_map(
        shards,
        mesh=split,
        in_specs=placed,
        out_specs=(P(EP + TP, None), P(EP, TP)),
        check_vma=False,
    )
```

```python
import math

import jax
import jax.numpy as jnp
from jax import lax
from jax.experimental import pallas as pl
from jax.experimental.pallas import tpu as pltpu
from jax.sharding import Mesh, PartitionSpec as P


NOPE = 64
ROPE = 32
VDIM = 64
EPSILON = 1e-06
EP = ("z", "c")
TP = ("y", "x")
F32 = jnp.float32
BF16 = jnp.bfloat16
MIB = 1 << 20


def params(mib):
    return pltpu.CompilerParams(vmem_limit_bytes=mib * MIB)


def turns(places, half):
    freqs = 10000.0 ** (-jnp.arange(half, dtype=F32) / half)
    angles = freqs[:, None] * places.astype(F32)[None, :]
    return jnp.cos(angles), jnp.sin(angles)


def dispatch_kernel(
    experts, room, at_ref, tokens_ref, gain_ref, routes_ref, out_ref, where_ref, row_ref
):
    rows, width = tokens_ref.shape
    share, pitch = out_ref.shape[2], 16 * (-(-room // 16))
    wide = tokens_ref[...].astype(F32)
    mean = jnp.sum(wide * wide, axis=-1, keepdims=True) * (1.0 / width)
    start = pl.multiple_of(at_ref[0] * share, share)
    row_ref[...] = gain_ref[...].astype(F32)[None, :]
    mine = tokens_ref[:, pl.ds(start, share)].astype(F32) * lax.rsqrt(mean + EPSILON)
    normed = (mine * row_ref[:, pl.ds(start, share)]).astype(BF16)
    names = lax.broadcasted_iota(jnp.int32, (experts, rows), 0)
    first, second = routes_ref[0:1, :], routes_ref[1:2, :]
    hit_first = jnp.where(names == first, 1.0, 0.0)
    hit_second = jnp.where(names == second, 1.0, 0.0)
    before = lax.broadcasted_iota(jnp.int32, (rows, rows), 0) < lax.broadcasted_iota(
        jnp.int32, (rows, rows), 1
    )
    earlier = jnp.where(before, 1.0, 0.0).astype(BF16)
    seen = jnp.dot((hit_first + hit_second).astype(BF16), earlier, preferred_element_type=F32)
    slot_first = jnp.sum(seen * hit_first, axis=0, keepdims=True)
    slot_second = jnp.sum(seen * hit_second, axis=0, keepdims=True)
    to_first = first * pitch + slot_first.astype(jnp.int32)
    to_second = second * pitch + slot_second.astype(jnp.int32)
    where_ref[0:1, :] = to_first
    where_ref[1:2, :] = to_second
    places = lax.broadcasted_iota(jnp.int32, (experts * pitch, rows), 0)
    chosen = jnp.where((places == to_first) | (places == to_second), 1.0, 0.0).astype(BF16)
    picked = jnp.dot(chosen, normed, preferred_element_type=F32).astype(BF16)
    out_ref[...] = picked.reshape(experts, pitch, share)[:, :room]


def dispatch(tokens, gain, routes, at, experts, room, share):
    rows = tokens.shape[0]
    vmem = pl.BlockSpec(memory_space=pltpu.VMEM)
    return pl.pallas_call(
        lambda *refs: dispatch_kernel(experts, room, *refs),
        out_shape=(
            jax.ShapeDtypeStruct((experts, room, share), BF16),
            jax.ShapeDtypeStruct((2, rows), jnp.int32),
        ),
        in_specs=[pl.BlockSpec(memory_space=pltpu.SMEM), vmem, vmem, vmem],
        out_specs=(vmem, vmem),
        scratch_shapes=[pltpu.VMEM((1, tokens.shape[1]), F32)],
        compiler_params=params(60),
        cost_estimate=pl.CostEstimate(flops=10_000_000, bytes_accessed=700_000, transcendentals=0),
        name="dispatch",
    )(at, tokens, gain, routes.T)


def expert_kernel(x_hbm, gate_hbm, up_hbm, down_hbm, out_ref, x_ref, gate_ref, up_ref, down_ref, gate_acc, up_acc, sems):
    pieces, rows, share = x_ref.shape
    step, few = 128, pieces // 4
    loads = []
    for n in range(4):
        some, deep = pl.ds(n * few, few), pl.ds(n * few * share, few * share)
        for m, (source, target, part) in enumerate(
            ((x_hbm, x_ref, some), (gate_hbm, gate_ref, deep), (up_hbm, up_ref, deep))
        ):
            loads.append(
                pltpu.make_async_copy(source.at[part], target.at[part], sems.at[3 * n + m])
            )
    loads.append(pltpu.make_async_copy(down_hbm, down_ref, sems.at[12]))
    for load in loads:
        load.start()
    for n in range(4):
        for load in loads[3 * n : 3 * n + 3]:
            load.wait()
        deep = pl.ds(n * few * share, few * share)
        for at in range(0, rows, step):
            x = jnp.concatenate(
                [x_ref[n * few + p, at : at + step, :] for p in range(few)], axis=1
            )
            gate = jnp.dot(x, gate_ref[deep, :], preferred_element_type=F32)
            up = jnp.dot(x, up_ref[deep, :], preferred_element_type=F32)
            if n:
                gate = gate + gate_acc[at : at + step, :]
                up = up + up_acc[at : at + step, :]
            gate_acc[at : at + step, :] = gate
            up_acc[at : at + step, :] = up
    loads[12].wait()
    for at in range(0, rows, step):
        gate, up = gate_acc[at : at + step, :], up_acc[at : at + step, :]
        hidden = (gate / (1.0 + jnp.exp(-gate)) * up).astype(BF16)
        for p in range(0, pieces, 2):
            term = jnp.dot(
                hidden, down_ref[:, p * share : (p + 2) * share], preferred_element_type=F32
            ).astype(BF16)
            out_ref[p, at : at + step, :] = term[:, :share]
            out_ref[p + 1, at : at + step, :] = term[:, share:]


def expert(x, gate, up, down):
    anywhere = pl.BlockSpec(memory_space=pl.ANY)
    return pl.pallas_call(
        expert_kernel,
        out_shape=jax.ShapeDtypeStruct(x.shape, BF16),
        in_specs=[anywhere] * 4,
        out_specs=pl.BlockSpec(memory_space=pltpu.VMEM),
        scratch_shapes=[pltpu.VMEM(w.shape, BF16) for w in (x, gate, up, down)]
        + [pltpu.VMEM((x.shape[1], gate.shape[1]), F32)] * 2
        + [pltpu.SemaphoreType.DMA((13,))],
        compiler_params=params(60),
        cost_estimate=pl.CostEstimate(flops=40_000_000, bytes_accessed=6_000_000, transcendentals=0),
        name="expert",
    )(x, gate, up, down)


def added_kernel(terms_ref, out_ref):
    count, room, _ = out_ref.shape
    few = 4
    for at in range(0, count, few):
        rows = pl.ds(at * room, few * room)
        total = terms_ref[0, rows, :].astype(F32)
        for n in range(1, terms_ref.shape[0]):
            total = total + terms_ref[n, rows, :].astype(F32)
        for k in range(few):
            out_ref[at + k] = total[k * room : (k + 1) * room].astype(BF16)


def added(terms, room):
    vmem = pl.BlockSpec(memory_space=pltpu.VMEM)
    return pl.pallas_call(
        added_kernel,
        out_shape=jax.ShapeDtypeStruct((terms.shape[1] // room, room, terms.shape[2]), BF16),
        in_specs=[vmem],
        out_specs=vmem,
        compiler_params=params(8),
        cost_estimate=pl.CostEstimate(flops=1_000_000, bytes_accessed=2_000_000, transcendentals=0),
        name="added",
    )(terms)


def combine_kernel(back_ref, where_ref, logits_ref, out_ref, wide_ref):
    rows, share = out_ref.shape
    wide_ref[...] = jnp.zeros_like(wide_ref)
    wide_ref[:, : back_ref.shape[1]] = back_ref[...]
    back = wide_ref[...].reshape(-1, share)
    places = lax.broadcasted_iota(jnp.int32, (rows, back.shape[0]), 1)
    left, right = logits_ref[:, 0:1], logits_ref[:, 1:2]
    top = jnp.maximum(left, right)
    grow_left, grow_right = jnp.exp(left - top), jnp.exp(right - top)
    both = grow_left + grow_right
    mixed = jnp.zeros(out_ref.shape, F32)
    for k, grown in ((0, grow_left), (1, grow_right)):
        chosen = jnp.where(places == where_ref[:, k : k + 1], 1.0, 0.0).astype(BF16)
        picked = jnp.dot(chosen, back, preferred_element_type=F32)
        mixed = mixed + picked * (grown / both)
    out_ref[...] = mixed.astype(BF16)


def combine(back, where, logits):
    vmem = pl.BlockSpec(memory_space=pltpu.VMEM)
    return pl.pallas_call(
        combine_kernel,
        out_shape=jax.ShapeDtypeStruct((logits.shape[0], back.shape[2]), BF16),
        in_specs=[vmem] * 3,
        out_specs=vmem,
        scratch_shapes=[pltpu.VMEM((back.shape[0], 16 * (-(-back.shape[1] // 16)), back.shape[2]), BF16)],
        compiler_params=params(8),
        name="combine",
    )(back, where, logits)


def normed_rows(ref, gain_ref):
    wide = ref[...].astype(F32)
    mean = jnp.sum(wide * wide, axis=-1, keepdims=True) * (1.0 / ref.shape[1])
    return (wide * lax.rsqrt(mean + EPSILON) * gain_ref[...].astype(F32)[None, :]).astype(BF16)


def across(left, right):
    return lax.dot_general(left, right, (((1,), (1,)), ((), ())), preferred_element_type=F32)


def turned(values, cosine, sine):
    half = values.shape[0] // 2
    first, second = values[:half], values[half:]
    return first * cosine - second * sine, first * sine + second * cosine


def keys_kernel(kv_ref, gain_ref, rope_ref, key_ref, value_ref, cos_ref, sin_ref, out_ref):
    normed = normed_rows(kv_ref, gain_ref)
    half = ROPE // 2
    first, second = turned(rope_ref[...].astype(F32), cos_ref[...], sin_ref[...])
    out_ref[:NOPE] = across(key_ref[...], normed).astype(BF16)
    out_ref[NOPE : NOPE + half] = first.astype(BF16)
    out_ref[NOPE + half : NOPE + ROPE] = second.astype(BF16)
    out_ref[NOPE + ROPE :] = across(value_ref[...], normed).astype(BF16)


def keys(kv, gain, rope_key, w_key, w_value, cosine, sine):
    vmem = pl.BlockSpec(memory_space=pltpu.VMEM)
    return pl.pallas_call(
        keys_kernel,
        out_shape=jax.ShapeDtypeStruct((NOPE + ROPE + VDIM, kv.shape[0]), BF16),
        in_specs=[vmem] * 7,
        out_specs=vmem,
        compiler_params=params(60),
        cost_estimate=pl.CostEstimate(flops=10_000_000, bytes_accessed=500_000, transcendentals=0),
        name="keys",
    )(kv, gain, rope_key.T, w_key.T, w_value.T, cosine, sine)


def queries_kernel(side, q_ref, gain_ref, nope_ref, rope_ref, cos_ref, sin_ref, out_ref):
    normed = normed_rows(q_ref, gain_ref)
    rows = normed.shape[0]
    few = rows // (side * side)
    order = [(y * side + x) * few for x in range(side) for y in range(side)]
    normed = jnp.concatenate([normed[at : at + few] for at in order], axis=0)
    half = ROPE // 2
    out_ref[:NOPE] = across(nope_ref[...], normed).astype(BF16)
    first, second = turned(across(rope_ref[...], normed), cos_ref[...], sin_ref[...])
    out_ref[NOPE : NOPE + half] = first.astype(BF16)
    out_ref[NOPE + half : NOPE + ROPE] = second.astype(BF16)
    out_ref[NOPE + ROPE :] = jnp.zeros((out_ref.shape[0] - NOPE - ROPE, rows), BF16)


def queries(q_latent, gain, w_nope, w_rope, cosine, sine, side):
    vmem = pl.BlockSpec(memory_space=pltpu.VMEM)
    return pl.pallas_call(
        lambda *refs: queries_kernel(side, *refs),
        out_shape=jax.ShapeDtypeStruct((128, q_latent.shape[0]), BF16),
        in_specs=[vmem] * 6,
        out_specs=vmem,
        compiler_params=params(24),
        cost_estimate=pl.CostEstimate(flops=10_000_000, bytes_accessed=700_000, transcendentals=0),
        name="queries",
    )(q_latent, gain, w_nope.T, w_rope.T, cosine, sine)


def attention_kernel(q_ref, kv_hbm, out_ref, kv_ref, s_ref, acc_ref, sems):
    tile = 256
    blocks, span = kv_hbm.shape[0] // 2, kv_ref.shape[2]
    queries = q_ref.shape[1]
    cut = NOPE + ROPE
    rate = (NOPE + ROPE) ** (-0.5) * math.log2(math.e)
    pad = jnp.zeros((q_ref.shape[0] - cut, tile), BF16)
    ones = jnp.ones((16, tile), BF16)
    tiles = [(part, at) for part in (0, 1) for at in range(0, span, tile)]
    halves = range(0, queries, tile)

    def load(block):
        source = pl.ds(2 * lax.rem(block, blocks), 2)
        return pltpu.make_async_copy(
            kv_hbm.at[source], kv_ref.at[pl.ds(2 * block, 2)], sems.at[block]
        )

    lead = 3
    for block in range(lead):
        load(jnp.int32(block)).start()

    def keys_of(block, n):
        part, at = tiles[n]
        return jnp.concatenate([kv_ref[2 * block + part, :cut, at : at + tile], pad], axis=0).T

    def scored(block, slot, n, h, most):
        s = jnp.dot(keys_of(block, n), q_ref[:, h : h + tile], preferred_element_type=F32)
        s_ref[slot, n * tile : (n + 1) * tile, h : h + tile] = s
        here = jnp.max(s.reshape(tile // 8, 8, tile), axis=0)
        return here if most is None else jnp.maximum(most, here)

    def absorbed(block, slot, n, h, top, total):
        part, at = tiles[n]
        s = s_ref[slot, n * tile : (n + 1) * tile, h : h + tile]
        weights = jnp.exp2((s - top) * rate).astype(BF16)
        rows = jnp.concatenate([kv_ref[2 * block + part, cut:, at : at + tile], ones], axis=0)
        return total + jnp.dot(rows, weights, preferred_element_type=F32)

    def topped(tops, top):
        block_top = jnp.max(jnp.concatenate(tops, axis=1), axis=0, keepdims=True)
        return jnp.maximum(top, block_top)

    def first_scores(top):
        tops = []
        for h in halves:
            most = None
            for n in range(len(tiles)):
                most = scored(0, 0, n, h, most)
            tops.append(most)
        return topped(tops, top)

    def pair(turn, carry):
        old_top, top = carry
        load(turn * 2 + 1).wait()
        load(turn * 2 + 2).wait()
        for after in (lead, lead + 1):

            @pl.when(turn * 2 + after <= blocks)
            def _():
                load(turn * 2 + after).start()

        for slot in (0, 1):
            block = turn * 2 + slot
            ahead = jnp.minimum(block + 1, blocks - 1)
            shrink = jnp.exp2((old_top - top) * rate)
            tops = []
            for h in halves:
                most, here = None, top[:, h : h + tile]
                total = acc_ref[:, h : h + tile] * shrink[:, h : h + tile]
                for n in range(len(tiles)):
                    most = scored(ahead, 1 - slot, n, h, most)
                    total = absorbed(block, slot, n, h, here, total)
                acc_ref[:, h : h + tile] = total
                tops.append(most)
            old_top, top = top, topped(tops, top)
        return old_top, top

    acc_ref[...] = jnp.zeros_like(acc_ref)
    floor = jnp.full((1, queries), -1e30, F32)
    load(jnp.int32(0)).wait()
    lax.fori_loop(0, blocks // 2, pair, (floor, first_scores(floor)))

    done = (acc_ref[:VDIM, :] / acc_ref[VDIM : VDIM + 1, :]).astype(BF16)
    for n in range(out_ref.shape[0]):
        out_ref[n] = done[:, n * out_ref.shape[2] : (n + 1) * out_ref.shape[2]]


def attention(q, kv, parts):
    vmem = pl.BlockSpec(memory_space=pltpu.VMEM)
    queries = q.shape[1]
    return pl.pallas_call(
        attention_kernel,
        out_shape=jax.ShapeDtypeStruct((parts, VDIM, queries // parts), BF16),
        in_specs=[vmem, pl.BlockSpec(memory_space=pl.ANY)],
        out_specs=vmem,
        scratch_shapes=[
            pltpu.VMEM((kv.shape[0] + 2, *kv.shape[1:]), BF16),
            pltpu.VMEM((2, 2 * kv.shape[2], queries), F32),
            pltpu.VMEM((VDIM + 16, queries), F32),
            pltpu.SemaphoreType.DMA((kv.shape[0] // 2 + 1,)),
        ],
        compiler_params=params(60),
        cost_estimate=pl.CostEstimate(flops=200_000_000, bytes_accessed=8_000_000, transcendentals=0),
        name="attention",
    )(q, kv)


def project_kernel(side, order_ref, heads_ref, *refs):
    packs, out_ref = refs[:side], refs[side]
    few, wide = out_ref.shape[1], 512
    queries = heads_ref.shape[2]
    spare = jnp.zeros((128 - VDIM, queries), F32)
    rows = []
    for k in range(side):
        mine = heads_ref[order_ref[k]].astype(F32)
        rows.append(jnp.concatenate([mine, spare], axis=0).T.astype(BF16)[:, :VDIM])
    for at in range(0, out_ref.shape[2], wide):
        total = jnp.zeros((queries, wide), F32)
        for k, pack in enumerate(packs):
            total = total + jnp.dot(
                rows[k], pack[:, at : at + wide], preferred_element_type=F32
            )
        total = total.astype(BF16)
        for y in range(out_ref.shape[0]):
            out_ref[y, :, at : at + wide] = total[y * few : (y + 1) * few]


def project_heads(heads, packs, order, few):
    vmem = pl.BlockSpec(memory_space=pltpu.VMEM)
    side, _, queries = heads.shape
    return pl.pallas_call(
        lambda *refs: project_kernel(side, *refs),
        out_shape=jax.ShapeDtypeStruct((queries // few, few, packs[0].shape[1]), BF16),
        in_specs=[pl.BlockSpec(memory_space=pltpu.SMEM)] + [vmem] * (1 + side),
        out_specs=vmem,
        compiler_params=params(16),
        cost_estimate=pl.CostEstimate(flops=10_000_000, bytes_accessed=2_000_000, transcendentals=0),
        name="heads",
    )(order, heads, *packs)


def ring(count, step):
    return [(i, (i + step) % count) for i in range(count)]


def from_row(value, axis):
    count = lax.axis_size(axis)
    return [value] + [lax.ppermute(value, axis, ring(count, k)) for k in range(1, count)]


def traded(pieces, axis):
    count, me = lax.axis_size(axis), lax.axis_index(axis)
    out = []
    for k in range(count):
        piece = lax.dynamic_index_in_dim(
            pieces, lax.rem(me + k, count), 0, False, allow_negative_indices=False
        )
        out.append(lax.ppermute(piece, axis, ring(count, k)) if k else piece)
    return out


def shards(
    q_latent,
    kv_latent,
    rope_key,
    q_gain,
    kv_gain,
    w_q_nope,
    w_q_rope,
    w_k_nope,
    w_value,
    w_out,
    tokens_b,
    norm_gain_b,
    routes,
    route_logits,
    w_gate,
    w_up,
    w_down,
):
    n_ep, n_tp = lax.axis_size(EP), lax.axis_size(TP)
    side = lax.axis_size("x")
    rows_b, width = tokens_b.shape
    room = 3 * rows_b // n_ep
    share = width // n_tp
    own_rows = q_latent.shape[0]
    first_row = lax.axis_index(EP) * own_rows
    places = jnp.arange(own_rows, dtype=jnp.int32)
    cos_k, sin_k = turns(first_row + places, ROPE // 2)
    piece = keys(kv_latent, kv_gain, rope_key, w_k_nope, w_value, cos_k, sin_k)
    gathered = lax.all_gather(piece, EP, axis=0, tiled=False)
    routes, places, piece = lax.optimization_barrier((routes, places, piece))
    outgoing, where = dispatch(
        tokens_b, norm_gain_b, routes, lax.axis_index(TP)[None], n_ep, room, share
    )
    arrived = lax.all_to_all(outgoing, EP, split_axis=0, concat_axis=0, tiled=True)
    w_parts = from_row(w_out, "x")
    order = lax.rem(lax.axis_index("x") + side - jnp.arange(side, dtype=jnp.int32), side)
    mixed = places.reshape(side, side, -1).transpose(1, 0, 2).reshape(-1)
    cos_q, sin_q = turns(first_row + mixed, ROPE // 2)
    q = queries(q_latent, q_gain, w_q_nope, w_q_rope, cos_q, sin_q, side)
    mine = arrived.reshape(1, n_ep * room, share)
    mine = jnp.broadcast_to(mine, (n_tp, n_ep * room, share))
    rows = lax.all_to_all(mine, TP, split_axis=0, concat_axis=0, tiled=True)
    terms = expert(rows, w_gate[0], w_up[0], w_down[0])
    terms = lax.all_to_all(terms, TP, split_axis=0, concat_axis=0, tiled=True)
    heads = attention(q, gathered, side)
    heads = lax.all_to_all(heads, "x", split_axis=0, concat_axis=0, tiled=True)
    partial = project_heads(heads, w_parts, order, own_rows // n_tp)
    partial = traded(partial, "y")
    finished = added(terms, room)
    back = lax.all_to_all(finished, EP, split_axis=0, concat_axis=0, tiled=True)
    expert_mix = combine(back, where.T, route_logits)
    mixer_out = sum(p.astype(F32) for p in partial).astype(BF16)
    return (mixer_out, expert_mix)


def solution(mesh):
    n_ep, n_tp = mesh.shape["ep"], mesh.shape["tp"]
    side = math.isqrt(n_tp)
    split = Mesh(
        mesh.devices.reshape(n_ep // 2, 2, side, n_tp // side), ("z", "c", "y", "x")
    )
    placed = (
        P(EP, None),
        P(EP, None),
        P(EP, None),
        P(),
        P(),
        P(None, TP),
        P(None, TP),
        P(None, TP),
        P(None, TP),
        P(TP, None),
        P(EP, None),
        P(),
        P(EP, None),
        P(EP, None),
        P(EP, None, TP),
        P(EP, None, TP),
        P(EP, TP, None),
    )
    return jax.shard_map(
        shards,
        mesh=split,
        in_specs=placed,
        out_specs=(P(EP + TP, None), P(EP, TP)),
        check_vma=False,
    )
```
